32 devices in a mesh: gr: 2 (over x), fs: 4 (over z), tp: 4 (over y, core).
Axes of the slice: x: 2, y: 2, z: 4, core: 2. Of those that a mesh axis runs over, the one named last changes fastest.
Arguments:
- prompt: bfloat16 [4096, 2048], P(('gr', 'fs')), may hold values from -6 to 6
- gain_first: float32 [2048], P(('gr', 'fs')), may hold values from 0.1 to 1.9
- gate_first: float32 [2048, 2816], P(('gr', 'fs'), 'tp'), may hold values from -0.125 to 0.125
- up_first: float32 [2048, 2816], P(('gr', 'fs'), 'tp'), may hold values from -0.125 to 0.125
- down_first: float32 [2816, 2048], P(('gr', 'fs'), 'tp'), may hold values from -0.109375 to 0.109375
- gain_second: float32 [2048], P(('gr', 'fs')), may hold values from 0.1 to 1.9
- gate_second: float32 [2048, 2816], P(('gr', 'fs'), 'tp'), may hold values from -0.125 to 0.125
- up_second: float32 [2048, 2816], P(('gr', 'fs'), 'tp'), may hold values from -0.125 to 0.125
- down_second: float32 [2816, 2048], P(('gr', 'fs'), 'tp'), may hold values from -0.109375 to 0.109375
Outputs:
- serve_gate_first: bfloat16 [2048, 2816], P(None, 'tp')
- serve_up_first: bfloat16 [2048, 2816], P(None, 'tp')
- serve_down_first: bfloat16 [2816, 2048], P('tp')
- serve_gate_second: bfloat16 [2048, 2816], P(None, 'tp')
- serve_up_second: bfloat16 [2048, 2816], P(None, 'tp')
- serve_down_second: bfloat16 [2816, 2048], P('tp')
- mixed: bfloat16 [4096, 2048], P(('gr', 'fs', 'tp'))
The draws below stay inside these ranges and needn't reach their ends.
All inputs are finite; a program needn't handle non-finite values.
Results may differ from the reference program's by a relative error of at most 0.0085.
Values may be sent and summed in bfloat16 or wider, within the bound.
No kernel may reach another device: no remote copies, remote signals or barrier semaphores. Data moves between devices by JAX's collectives and lax.ppermute only.
A program may use at most 128 MiB of HBM per device.

```python
import jax
import jax.numpy as jnp
from jax import lax

D = 2048
FF = 2816
TOKENS = 4096
N_TP = 4


def shard_levels(stream_key, dims, pieces, low, high):
    def one(dim, shards_of):
        steps = jax.random.uniform(jax.random.fold_in(jax.random.fold_in(stream_key, 6), dim), (shards_of,), jnp.float32, low / len(pieces), high / len(pieces))
        return jnp.repeat(jnp.exp(steps), dims[dim] // shards_of).reshape((-1,) + (1,) * (len(dims) - dim - 1))

    level = one(*pieces[0])
    for cut in pieces[1:]:
        level = level * one(*cut)
    return level


def normal_values(stream_key, shape, scale, most, pieces=(), dtype=jnp.bfloat16):
    gain = shard_levels(stream_key, shape, pieces, -0.22, 0.18) if pieces else 1.0
    result = jax.random.normal(stream_key, shape, jnp.float32) * scale * gain
    return jnp.minimum(jnp.maximum(result, -most), most).astype(dtype)


def setup_inputs(seed: int = 0) -> dict:
    keys = jax.random.split(jax.random.key(seed), 10)
    prompt = normal_values(keys[0], (TOKENS, D), 1.0, 6.0, ((0, 8),))
    gain_first = jnp.clip(1.0 + 0.18 * jax.random.normal(keys[1], (D,), jnp.float32), 0.1, 1.9)
    gate_first = normal_values(keys[2], (D, FF), D ** -0.5, 0.125, ((0, 8), (1, 4)), jnp.float32)
    up_first = normal_values(keys[3], (D, FF), D ** -0.5, 0.125, ((0, 8), (1, 4)), jnp.float32)
    down_first = normal_values(keys[4], (FF, D), FF ** -0.5, 0.109375, ((0, 8), (1, 4)), jnp.float32)
    gain_second = jnp.clip(1.0 + 0.18 * jax.random.normal(keys[5], (D,), jnp.float32), 0.1, 1.9)
    gate_second = normal_values(keys[6], (D, FF), D ** -0.5, 0.125, ((0, 8), (1, 4)), jnp.float32)
    up_second = normal_values(keys[7], (D, FF), D ** -0.5, 0.125, ((0, 8), (1, 4)), jnp.float32)
    down_second = normal_values(keys[8], (FF, D), FF ** -0.5, 0.109375, ((0, 8), (1, 4)), jnp.float32)
    return dict(prompt=prompt, gain_first=gain_first, gate_first=gate_first, up_first=up_first, down_first=down_first, gain_second=gain_second, gate_second=gate_second, up_second=up_second, down_second=down_second)


def normalize(rows):
    rows = rows.astype(jnp.float32)
    scale = jax.lax.rsqrt(lax.optimization_barrier(jnp.mean(rows * rows, axis=-1, keepdims=True)) + 1e-06)
    return (rows * scale).astype(jnp.bfloat16)

def layer_branch(normed, w_gate, w_up, w_down):
    gate = jnp.dot(normed, w_gate, preferred_element_type=jnp.float32)
    upper = jnp.dot(normed, w_up, preferred_element_type=jnp.float32)
    hidden = (jax.nn.silu(gate) * upper).astype(jnp.bfloat16)
    width = hidden.shape[1] // N_TP
    total = jnp.zeros((hidden.shape[0], w_down.shape[1]), jnp.float32)
    for block in range(N_TP):
        part = jnp.dot(hidden[:, block * width:(block + 1) * width], w_down[block * width:(block + 1) * width, :], preferred_element_type=jnp.float32)
        total = total + part.astype(jnp.bfloat16).astype(jnp.float32)
    return total

def reference(prompt, gain_first, gate_first, up_first, down_first, gain_second, gate_second, up_second, down_second):
    serve_gate_first = (gain_first[:, None] * gate_first).astype(jnp.bfloat16)
    serve_up_first = (gain_first[:, None] * up_first).astype(jnp.bfloat16)
    serve_down_first = down_first.astype(jnp.bfloat16)
    serve_gate_second = (gain_second[:, None] * gate_second).astype(jnp.bfloat16)
    serve_up_second = (gain_second[:, None] * up_second).astype(jnp.bfloat16)
    serve_down_second = down_second.astype(jnp.bfloat16)
    stream = prompt.astype(jnp.float32) + 0.5 * layer_branch(normalize(prompt), serve_gate_first, serve_up_first, serve_down_first)
    mixed = (stream + 0.5 * layer_branch(normalize(stream), serve_gate_second, serve_up_second, serve_down_second)).astype(jnp.bfloat16)
    return (serve_gate_first, serve_up_first, serve_down_first, serve_gate_second, serve_up_second, serve_down_second, mixed)
```

```python
import jax
import jax.numpy as jnp
from jax import lax
from jax.experimental import pallas as pl
from jax.experimental.pallas import tpu as pltpu
from jax.sharding import PartitionSpec as P


RING = ("gr", "fs")
BF = jnp.bfloat16
F32 = jnp.float32
VMEM = pl.BlockSpec(memory_space=pltpu.VMEM)
SMEM = pl.BlockSpec(memory_space=pltpu.SMEM)
PARAMS = pltpu.CompilerParams(vmem_limit_bytes=48 * 1024 * 1024)


def snake(index, width):
    row, col = index // width, index % width
    if isinstance(index, int):
        return row * width + (col if row % 2 == 0 else width - 1 - col)
    return row * width + jnp.where(row % 2 == 0, col, width - 1 - col)


def normalize(rows):
    scale = lax.rsqrt(jnp.mean(rows * rows, axis=-1, keepdims=True) + 1e-06)
    return (rows * scale).astype(BF)


def place(blocks, where, turned):
    wide, rows = blocks[0].shape if turned else blocks[0].shape[::-1]
    shape = (len(blocks) * rows, wide)
    if rows % (128 if turned else 16):
        out = jnp.zeros(shape, BF)
        for i, block in enumerate(blocks):
            block = block.T if turned else block
            out = lax.dynamic_update_slice_in_dim(out, block, where[i] * rows, 0)
        return out

    def body(at, *refs):
        out = refs[-1]
        for i, ref in enumerate(refs[:-1]):
            start = pl.multiple_of(at[i] * rows, rows)
            out[pl.ds(start, rows), :] = ref[...].T if turned else ref[...]

    return pl.pallas_call(
        body,
        out_shape=jax.ShapeDtypeStruct(shape, BF),
        in_specs=[SMEM] + [VMEM] * len(blocks),
        out_specs=VMEM,
        compiler_params=PARAMS,
        cost_estimate=pl.CostEstimate(
            flops=1000000000, transcendentals=0, bytes_accessed=4 * shape[0] * shape[1]
        ),
        name="place",
    )(where, *blocks)


def project(normed, gates, gates_at, ups, ups_at, sums, finish):
    tokens, (units, rows) = normed.shape[0], gates[0].shape
    n, m = len(gates), len(ups)

    def body(at, x, *refs):
        weights, refs = refs[: n + m], refs[n + m :]
        if sums is not None:
            before, refs = refs[:2], refs[2:]
        totals = []
        for low, high in ((0, n), (n, n + m)):
            total = None
            for i in range(low, high):
                start = pl.multiple_of(at[i] * rows, rows)
                term = lax.dot_general(
                    x[:, pl.ds(start, rows)],
                    weights[i][...],
                    (((1,), (1,)), ((), ())),
                    preferred_element_type=F32,
                )
                total = term if total is None else total + term
            if sums is not None:
                total = total + before[len(totals)][...]
            totals.append(total)
        if finish:
            gate, upper = totals
            refs[0][...] = (gate / (1.0 + jnp.exp(-gate)) * upper).astype(BF)
        else:
            refs[0][...], refs[1][...] = totals

    one = jax.ShapeDtypeStruct((tokens, units), BF if finish else F32)
    return pl.pallas_call(
        body,
        out_shape=one if finish else (one, one),
        in_specs=[SMEM] + [VMEM] * (1 + n + m + (0 if sums is None else 2)),
        out_specs=VMEM if finish else (VMEM, VMEM),
        compiler_params=PARAMS,
        cost_estimate=pl.CostEstimate(
            flops=2 * tokens * units * rows * (n + m),
            transcendentals=0,
            bytes_accessed=2 * units * rows * (n + m),
        ),
        name="project",
    )(jnp.concatenate([gates_at, ups_at]), normed, *gates, *ups, *(sums or ()))


def solution(mesh):
    outer, inner, wide = (mesh.shape[a] for a in ("gr", "fs", "tp"))
    count = outer * inner
    bits = wide.bit_length() - 1
    if wide != 1 << bits or bits < 1:
        raise ValueError("tp size")
    ring = [snake(i, inner) for i in range(count)]
    ahead = [(ring[i], ring[(i + 1) % count]) for i in range(count)]
    back = [(ring[i], ring[i - 1]) for i in range(count)]
    short = (count - 1) // 2
    long = count - 1 - short

    def gather(block, forward):
        limits = (long, short) if forward else (short, long)
        found = {0: block}
        for step in range(1, long + 1):
            for sign, pairs, limit in ((1, ahead, limits[0]), (-1, back, limits[1])):
                if step <= limit:
                    found[sign * step] = lax.ppermute(found[sign * (step - 1)], RING, pairs)
        return found

    def swap(x, bit):
        return lax.ppermute(x, "tp", [(t, t ^ (1 << bit)) for t in range(wide)])

    def shards(prompt, gain_a, gate_a, up_a, down_a, gain_b, gate_b, up_b, down_b):
        here = snake(lax.axis_index("gr") * inner + lax.axis_index("fs"), inner)
        me = lax.axis_index("tp")

        def origin(distances):
            return jnp.stack([snake((here - d) % count, inner) for d in distances])

        def bit_of(b):
            return (me >> b) & 1

        def fold(gain, weight):
            return (gain[:, None] * weight).astype(BF).T

        def after(values, found):
            tied = lax.optimization_barrier(
                tuple(values) + tuple(f[s * short] for f in found for s in (1, -1))
            )
            return tied[: len(values)]

        def exchange(found):
            full = place(list(found.values()), origin(list(found)), False)
            rows, cols = full.shape[0] // wide, full.shape[1]
            out = jnp.zeros((rows, wide * cols), BF)
            for d in range(wide):
                to = me ^ d
                piece = lax.dynamic_slice_in_dim(full, to * rows, rows, 0)
                if d:
                    piece = lax.ppermute(piece, "tp", [(t, t ^ d) for t in range(wide)])
                out = lax.dynamic_update_slice_in_dim(out, piece, to * cols, 1)
            return out

        def hidden_units(normed, gates, ups):
            spans = (list(gates), list(ups))
            rows = gates[0].shape[1]
            serve = [place(list(f.values()), origin(list(f)), True) for f in (gates, ups)]
            if rows % 128:
                gate, upper = (jnp.dot(normed, w, preferred_element_type=F32) for w in serve)
                return (jax.nn.silu(gate) * upper).astype(BF), serve
            first = [[d for d in spans[0] if abs(d) <= short], [d for d in spans[1] if abs(d) < short]]
            rest = [[d for d in spans[i] if d not in first[i]] for i in (0, 1)]
            sums = None
            for picks, finish in ((first, False), (rest, True)):
                sums = project(
                    normed,
                    [gates[d] for d in picks[0]],
                    origin(picks[0]),
                    [ups[d] for d in picks[1]],
                    origin(picks[1]),
                    sums,
                    finish,
                )
            return sums, serve

        def own_sum(hidden, down):
            half = hidden.shape[0] // 2
            per = hidden.shape[0] // wide
            top = bits - 1
            sides = []
            for side in (1 - bit_of(top), bit_of(top)):
                rows = lax.dynamic_slice_in_dim(hidden, side * half, half, 0)
                term = jnp.dot(rows, down, preferred_element_type=F32).astype(BF)
                term = term.reshape(wide // 2, per, -1)
                for b in range(top):
                    pair = term.reshape(term.shape[0] // 2, 2, per, -1)
                    keep = lax.dynamic_index_in_dim(pair, bit_of(b), 1, False)
                    send = lax.dynamic_index_in_dim(pair, 1 - bit_of(b), 1, False)
                    term = keep.astype(F32) + swap(send.astype(BF), b).astype(F32)
                sides.append(term[0])
            return sides[1].astype(F32) + swap(sides[0].astype(BF), top).astype(F32)

        def all_rows(own):
            for b in reversed(range(bits)):
                other = swap(own, b)
                own = jnp.where(
                    bit_of(b) == 0,
                    jnp.stack([own, other]),
                    jnp.stack([other, own]),
                )
            own = own.transpose(tuple(reversed(range(bits))) + (bits, bits + 1))
            return own.reshape(-1, own.shape[-1])

        tall_a = gather(down_a.astype(BF), True)
        tall_b = gather(down_b.astype(BF), False)
        g_a, u_a = after((fold(gain_a, gate_a), fold(gain_a, up_a)), (tall_a, tall_b))
        gates_a, ups_a = gather(g_a, True), gather(u_a, False)
        g_b, u_b = after((fold(gain_b, gate_b), fold(gain_b, up_b)), (gates_a, ups_a))
        gates_b, ups_b = gather(g_b, True), gather(u_b, False)

        out_down_a, out_down_b = exchange(tall_a), exchange(tall_b)
        normed_a = normalize(prompt.astype(F32))
        hidden_a, (out_gate_a, out_up_a) = hidden_units(normed_a, gates_a, ups_a)
        per = prompt.shape[0] // wide
        own = lax.dynamic_slice_in_dim(prompt, me * per, per, 0).astype(F32)
        stream = own + 0.5 * own_sum(hidden_a, out_down_a)
        normed_b = all_rows(normalize(stream))
        hidden_b, (out_gate_b, out_up_b) = hidden_units(normed_b, gates_b, ups_b)
        mixed = (stream + 0.5 * own_sum(hidden_b, out_down_b)).astype(BF)
        return (out_gate_a, out_up_a, out_down_a, out_gate_b, out_up_b, out_down_b, mixed)

    split, lone = P(RING, "tp"), P(RING)
    return jax.shard_map(
        shards,
        mesh=mesh,
        in_specs=(P(RING, None), lone, split, split, split, lone, split, split, split),
        out_specs=(
            P(None, "tp"),
            P(None, "tp"),
            P("tp", None),
            P(None, "tp"),
            P(None, "tp"),
            P("tp", None),
            P(("gr", "fs", "tp"), None),
        ),
        check_vma=False,
    )
```
